512 devices in a mesh: ep: 32 (over z, x), tp: 16 (over y, core).
Axes of the slice: x: 4, y: 8, z: 8, core: 2. Of those that a mesh axis runs over, the one named last changes fastest.
Arguments:
- tokens: bfloat16 [256, 2048], P('ep', 'tp'), may hold values from -10 to 10, as said below
- norm_gain: float32 [2048], P('tp'), may hold values from 0.5 to 1.5
- norm_bias: float32 [2048], P('tp'), may hold values from -0.3 to 0.3
- group_pick: int32 [256, 1], P('ep'), may hold values from 0 to 7; in each aligned block of 8 rows (0 to 7, 8 to 15, ...) at most 2 rows name the same one
- member_pick: int32 [256, 4], P('ep'), may hold values from 0 to 7, all different within a row
- picked_probs: float32 [256, 4], P('ep'), may hold values from 0.05 to 1
- gate_weight: bfloat16 [64, 2048, 1024], P('ep', 'tp'), may hold values from -0.125 to 0.125
- up_weight: bfloat16 [64, 2048, 1024], P('ep', 'tp'), may hold values from -0.125 to 0.125
- down_weight: bfloat16 [64, 1024, 2048], P('ep', None, 'tp'), may hold values from -0.375 to 0.375
Outputs:
- mixed: bfloat16 [256, 2048], P('ep', 'tp')
The draws below stay inside these ranges and needn't reach their ends.
Inputs may be any that keep to these rules, and one draw needn't show every extreme that they name: `group_pick`: each entry is a group number from 0 to 7; within each aligned block of 8 tokens no group is named by more than 2 tokens, a bound that some block reaches. `member_pick`: each token's 4 entries are different member numbers from 0 to 7. `tokens`: each token is its own offset between -2 and 2 plus its own scale between 0.25 and 2 times entries of at most 4 in size.
All inputs are finite; a program needn't handle non-finite values.
Results may differ from the reference program's by a relative error of at most 0.01.
Values may be sent and summed in bfloat16 or wider, within the bound.
A program may use at most 64 MiB of HBM per device.

```python
import math
import jax
import jax.numpy as jnp
import numpy as np
from jax import lax

D = 2048
FF = 1024
EPG = 8
TOP_K = 4
TOK_DEV = 8
TOKENS = 256
EXPERTS = 64
GROUPS = 8
GCAP = 2


def draw_tokens(key, part):
    offset_key, scale_key, noise_key = jax.random.split(key, 3)
    offsets = jax.random.uniform(offset_key, (TOKENS, 1), jnp.float32, -2.0, 2.0)
    logs = jax.random.uniform(scale_key, (TOKENS, 1), jnp.float32, math.log(0.5), math.log(2.0))
    noise = jnp.clip(jax.random.normal(noise_key, (TOKENS, D), jnp.float32), -4.0, 4.0)
    return (offsets + jnp.exp(logs) * noise).astype(jnp.bfloat16)


def level_of(key, extent, cuts, smallest, largest):
    def one(dim, parts):
        heights = jax.random.uniform(jax.random.fold_in(jax.random.fold_in(key, 6), dim), (parts,), jnp.float32, smallest / len(cuts), largest / len(cuts))
        return jnp.repeat(jnp.exp(heights), extent[dim] // parts).reshape((-1,) + (1,) * (len(extent) - dim - 1))

    factor_of = one(*cuts[0])
    for cut in cuts[1:]:
        factor_of = factor_of * one(*cut)
    return factor_of


def picks_of(stream_key, rows, count, top, lift):
    sequence = jax.random.permutation(jax.random.fold_in(stream_key, 1), count)
    favour = sequence
    for power in range(3):
        favour = favour * favour // count
    favour = favour * lift // count
    tickets = jax.random.randint(jax.random.fold_in(stream_key, 2), (rows, count), 0, 4096) + favour
    fixed_rows = jax.random.permutation(jax.random.fold_in(stream_key, 3), rows)[jnp.arange(count) % rows]
    tickets = jnp.where(jnp.arange(rows)[:, None] == fixed_rows[None, :], 1 << 14, tickets)
    score = tickets * count + jnp.arange(count)
    return lax.top_k(score.astype(jnp.int32), top)[1].astype(jnp.int32)


def routed_block(stream_key, own, number, rows, number_of, top, most, lean):
    ranking = jax.random.permutation(stream_key, number_of)
    heavy_load, usual = portions_of(number_of, rows * top, most, lean, True), portions_of(number_of, rows * top, most, lean, False)
    places = jnp.arange(number_of)

    def named(tallies, turn):
        used = int((tallies > 0).sum())
        fixed = max(1, used // 4)
        moved = fixed + (places - fixed + turn * (used - fixed)) % max(1, number_of - fixed)
        return jnp.zeros((number_of,), jnp.int32).at[ranking[jnp.where(places < fixed, places, moved)]].set(jnp.asarray(tallies, jnp.int32))

    tallies = jnp.where(number % 4 == 0, named(heavy_load, number // 4), named(usual, number - number // 4 - 1))
    mixed = jax.random.permutation(jax.random.fold_in(own, 3), number_of)
    source_of, sink = mixed[0:number_of // 2 * 2:2], mixed[1:number_of // 2 * 2:2]
    room = jnp.minimum(tallies[source_of] - 1, most - tallies[sink]) // 2
    room = jnp.where((source_of == ranking[0]) | (sink == ranking[0]) | (tallies[sink] == 0), 0, jnp.maximum(room, 0))
    moved = jax.random.randint(jax.random.fold_in(own, 4), (number_of // 2,), 0, 1 << 20) % (room + 1)
    tallies = tallies.at[source_of].add(-moved).at[sink].add(moved)
    items = jnp.searchsorted(jnp.cumsum(tallies), jnp.arange(rows * top), side="right").astype(jnp.int32)
    grid = items.reshape(top, rows).T
    grid = grid[jax.random.permutation(jax.random.fold_in(own, 1), rows)]
    turn = jax.random.randint(jax.random.fold_in(own, 2), (rows, 1), 0, top)
    return jnp.take_along_axis(grid, (jnp.arange(top)[None, :] + turn) % top, axis=1)


def portions_of(amount, total, bound, lean, full):
    portions = [(1 << 20) // math.isqrt(standing ** lean) + 1 for standing in range(1, amount + 1)]
    largest = bound if full else min(bound, max(-(-total // amount), total * portions[0] // sum(portions)))
    least = 1 if total - largest >= amount - 1 else 0
    given, surplus = [largest] + [least] * (amount - 1), total - largest - least * (amount - 1)
    while surplus > 0:
        free = [i for i in range(1, amount) if given[i] < largest] or [i for i in range(1, amount) if given[i] < bound]
        whole, left = sum([portions[i] for i in free]), surplus
        for i in free:
            extra = min(bound - given[i], max(1, left * portions[i] // whole), surplus)
            given[i] = given[i] + extra
            surplus = surplus - extra
    return np.array(given)


def scatter_about(stream_key, dims, scale, limit, cuts=(), held_as=jnp.bfloat16):
    factor_of = level_of(stream_key, dims, cuts, -0.22, 0.18) if cuts else 1.0
    drawn = jax.random.normal(stream_key, dims, jnp.float32) * scale * factor_of
    return jnp.minimum(jnp.maximum(drawn, -limit), limit).astype(held_as)


def setup_inputs(seed: int = 0) -> dict:
    arg_keys = jax.random.split(jax.random.key(seed), 10)
    tokens = draw_tokens(jax.random.fold_in(arg_keys[9], 71), 0)
    norm_gain = jnp.clip(1.0 + 0.1 * jax.random.normal(arg_keys[1], (D,), jnp.float32), 0.5, 1.5)
    norm_bias = scatter_about(arg_keys[2], (D,), 0.1, 0.3, ((0, 16),), jnp.float32)
    group_pick_keys = jax.random.split(jax.random.fold_in(arg_keys[3], 1), TOKENS // TOK_DEV)
    group_pick_turns = jax.random.permutation(jax.random.fold_in(arg_keys[3], 3), TOKENS // TOK_DEV)
    group_pick = jax.vmap(lambda own, number: routed_block(jax.random.fold_in(arg_keys[3], 2), own, number, TOK_DEV, GROUPS, 1, GCAP, 2))(group_pick_keys, group_pick_turns).reshape((TOKENS, 1))
    member_pick = picks_of(arg_keys[4], TOKENS, EPG, TOP_K, 4096)
    picked_probs = jnp.clip(jnp.exp(math.log(1.0) - 2.9957323 * jax.random.uniform(arg_keys[5], (TOKENS, TOP_K), jnp.float32) ** level_of(arg_keys[5], (TOKENS, TOP_K), ((0, 32),), -0.2, 0.2)), 0.05, 1.0)
    gate_weight = scatter_about(arg_keys[6], (EXPERTS, D, FF), D ** -0.5, 0.125, ((0, 32), (1, 16)))
    up_weight = scatter_about(arg_keys[7], (EXPERTS, D, FF), D ** -0.5, 0.125, ((0, 32), (1, 16)))
    down_weight = scatter_about(arg_keys[8], (EXPERTS, FF, D), (FF // 4) ** -0.5, 0.375, ((0, 32), (2, 16)))
    return {"tokens": tokens, "norm_gain": norm_gain, "norm_bias": norm_bias, "group_pick": group_pick, "member_pick": member_pick, "picked_probs": picked_probs, "gate_weight": gate_weight, "up_weight": up_weight, "down_weight": down_weight}


norm_epsilon = 1e-5


def reference(tokens, norm_gain, norm_bias, group_pick, member_pick, picked_probs, gate_weight, up_weight, down_weight):
    values = tokens.astype(jnp.float32)
    center = jnp.mean(values, axis=1, keepdims=True)
    shifted = values - center
    spread = jnp.mean(shifted * shifted, axis=1, keepdims=True)
    scaled = shifted * lax.rsqrt(spread + norm_epsilon)
    normed = (scaled * norm_gain.astype(jnp.float32) + norm_bias.astype(jnp.float32)).astype(jnp.bfloat16)
    chosen = (group_pick * EPG + member_pick).astype(jnp.int32)
    shares = picked_probs / jnp.sum(picked_probs, axis=1, keepdims=True)

    def one_token(packed):
        row, picks, weights = packed
        row_wide = row.astype(jnp.float32)
        gate_rows = jnp.take(gate_weight, picks, axis=0).astype(jnp.float32)
        up_rows = jnp.take(up_weight, picks, axis=0).astype(jnp.float32)
        down_rows = jnp.take(down_weight, picks, axis=0).astype(jnp.float32)
        gate_sum = jnp.einsum("d,kdf->kf", row_wide, gate_rows)
        up_sum = jnp.einsum("d,kdf->kf", row_wide, up_rows)
        hidden = (jax.nn.silu(gate_sum) * up_sum).astype(jnp.bfloat16)
        expert_out = jnp.einsum("kf,kfd->kd", hidden.astype(jnp.float32), down_rows).astype(jnp.bfloat16)
        return jnp.sum(weights[:, None] * expert_out.astype(jnp.float32), axis=0)

    combined = lax.map(one_token, (normed, chosen, shares))
    return combined.astype(jnp.bfloat16)
```

```python
import functools

import jax
import jax.numpy as jnp
from jax import lax
from jax.experimental import pallas as pl
from jax.experimental.pallas import tpu as pltpu
from jax.sharding import PartitionSpec as P

EPG = 8
CORES = 2
LANES = 128
ROW_CHIPS = 4
norm_epsilon = 1e-05
MESH = pl.DeviceIdType.MESH
F32 = jnp.float32
BF16 = jnp.bfloat16


def iota(shape, dim):
    return lax.broadcasted_iota(jnp.int32, shape, dim)


def around(d, size):
    return min(d, size - d)


def kernel(
    E, T, G, cap,
    tokens_h, gain_h, bias_h, group_h, member_h, probs_h, gate_h, up_h, down_h,
    out_ref,
    tokens_v, gain_v, bias_v, group_v, member_v, probs_v, gate_v, up_v, down_v,
    stats_out, stats_in, rows_out, rows_in, rows_all, info_all,
    core_out, core_in, y_out, y_in, hid_own, hid_other, back_out, back_in,
    local_sem, weight_sem,
    stats_s, stats_r, rows_s, rows_r,
    core_s, core_r, y_s, y_r, hid_s, hid_r, pass_s, pass_r, back_s, back_r,
):
    n, width = tokens_h.shape
    LE = gate_h.shape[0]
    FF = gate_h.shape[2]
    half = FF // CORES
    quarters = half // LANES
    NY = T // CORES
    R = E * cap
    rows_each = cap + 2
    group_devices = EPG // LE
    X = ROW_CHIPS
    Z = E // X
    me = lax.axis_index("ep")
    mt = lax.axis_index("tp")
    core = lax.rem(mt, CORES)
    my = lax.div(mt, CORES)
    mz = lax.div(me, X)
    mx = lax.rem(me, X)
    partner = my * CORES + (1 - core)

    def peer(d):
        dz, dx = divmod(d, X)
        return lax.rem(mz + dz, Z) * X + lax.rem(mx + dx, X)

    def source(d):
        dz, dx = divmod(d, X)
        return lax.rem(mz + Z - dz, Z) * X + lax.rem(mx + X - dx, X)

    def remote(src, dst, ssem, rsem, ep, tp):
        return pltpu.make_async_remote_copy(
            src_ref=src, dst_ref=dst, send_sem=ssem, recv_sem=rsem,
            device_id=(ep, tp), device_id_type=MESH,
        )

    ep_order = sorted(range(1, E), key=lambda d: -(around(d // X, Z) + around(d % X, X)))
    y_order = sorted(range(1, NY), key=lambda o: -around(o, NY))
    tp_order = sorted(range(1, T), key=lambda t: -around(t // CORES, NY))

    def tp_at(t):
        return lax.rem(my + t // CORES, NY) * CORES + lax.rem(core + t % CORES, CORES)

    def y_at(o):
        return lax.rem(my + o, NY)

    eps = {d: peer(d) for d in ep_order}
    tps = {t: tp_at(t) for t in tp_order}

    barrier = pltpu.get_barrier_semaphore()
    for d in ep_order:
        pl.semaphore_signal(barrier, inc=1, device_id=(eps[d], mt), device_id_type=MESH)
    for t in tp_order:
        pl.semaphore_signal(barrier, inc=1, device_id=(me, tps[t]), device_id_type=MESH)

    small = [
        pltpu.make_async_copy(h, v, local_sem.at[i])
        for i, (h, v) in enumerate(
            ((tokens_h, tokens_v), (group_h, group_v), (member_h, member_v), (probs_h, probs_v),
             (gain_h, gain_v), (bias_h, bias_v))
        )
    ]
    for c in small:
        c.start()
    weights = [
        [pltpu.make_async_copy(h.at[j], v.at[j], weight_sem.at[w, j]) for j in range(LE)]
        for w, (h, v) in enumerate(((gate_h, gate_v), (up_h, up_v), (down_h, down_v)))
    ]
    for w in range(3):
        for j in range(LE):
            weights[w][j].start()
    for c in small:
        c.wait()

    lane = iota((n, n), 1)
    sub = iota((n, n), 0)
    spot = iota((n, LANES), 1)
    spot_sub = iota((n, LANES), 0)

    values = tokens_v[...].astype(F32)
    center_here = jnp.sum(values, axis=1, keepdims=True) / width
    away = values - center_here
    square_here = jnp.sum(away * away, axis=1, keepdims=True)
    stats = jnp.where(spot == spot_sub, center_here, 0.0)
    stats += jnp.where(spot == spot_sub + n, square_here, 0.0)
    stats_row = jnp.sum(stats, axis=0, keepdims=True)
    stats_out[...] = stats_row

    def column(row):
        wide = jnp.broadcast_to(row, (n, n))
        return jnp.sum(jnp.where(lane == sub, wide, 0.0), axis=1, keepdims=True)

    group_row = group_v[...].astype(F32)
    group_col = column(group_row)
    same = jnp.where(group_col == group_row, 1.0, 0.0)
    slot_row = jnp.sum(jnp.where(sub < lane, same, 0.0), axis=0, keepdims=True)
    slot_col = jnp.sum(jnp.where(lane < sub, same, 0.0), axis=1, keepdims=True)
    key_col = group_col * cap + slot_col

    probs = probs_v[...]
    member = member_v[...].astype(F32)
    shares = probs / jnp.sum(probs, axis=0, keepdims=True)
    spot_f = spot.astype(F32)
    info = jnp.zeros((n, LANES), F32)
    for k in range(probs.shape[0]):
        hit = spot_f == column(member[k : k + 1, :]) * cap + slot_col
        info += jnp.where(hit, column(shares[k : k + 1, :]), 0.0)
    high = info.astype(BF16).astype(F32)
    low = info - high

    packed_row = iota((G * rows_each, n), 0).astype(F32)
    place = jnp.where(packed_row == group_row * rows_each + slot_row, 1.0, 0.0)
    place_high = jnp.where(packed_row == group_row * rows_each + cap, 1.0, 0.0)
    place_low = jnp.where(packed_row == group_row * rows_each + (cap + 1), 1.0, 0.0)
    base = jnp.zeros((G * rows_each, LANES), F32)
    for t in range(n):
        base += place_high[:, t : t + 1] * high[t : t + 1, :]
        base += place_low[:, t : t + 1] * low[t : t + 1, :]
    gain = gain_v[...]
    bias = bias_v[...]

    pl.semaphore_wait(barrier, E + T - 2)

    told = []
    for t in tp_order:
        c = remote(stats_out, stats_in.at[t], stats_s.at[t], stats_r.at[t], me, tps[t])
        c.start()
        told.append(c)
    for c in told:
        c.wait_recv()
    heard = [stats_row] + [stats_in[t] for t in range(1, T)]
    total = heard[0]
    for h in heard[1:]:
        total += h
    middle = total / T
    moved = jnp.zeros((1, LANES), F32)
    for h in heard:
        moved += (h - middle) * (h - middle)
    middle_wide = jnp.broadcast_to(middle, (n, LANES))
    total_wide = jnp.broadcast_to(total, (n, LANES))
    moved_wide = jnp.broadcast_to(moved, (n, LANES))
    center = jnp.sum(jnp.where(spot == spot_sub, middle_wide, 0.0), axis=1, keepdims=True)
    square = jnp.sum(
        jnp.where(spot == spot_sub + n, total_wide, 0.0)
        + jnp.where(spot == spot_sub, width * moved_wide, 0.0),
        axis=1, keepdims=True,
    )
    spread = square / (width * T)
    normed = (values - center) * lax.rsqrt(spread + norm_epsilon) * gain + bias
    packed = base
    for t in range(n):
        packed += place[:, t : t + 1] * normed[t : t + 1, :]
    for g in range(G):
        rows_out[g] = packed[g * rows_each : (g + 1) * rows_each, :].astype(BF16)

    sent = []
    for d in ep_order:
        c = remote(
            rows_out.at[lax.div(eps[d], group_devices)], rows_in.at[d],
            rows_s.at[d], rows_r.at[d], eps[d], mt,
        )
        c.start()
        sent.append(c)
    rows_in[0] = rows_out[lax.div(me, group_devices)]
    for w in range(2):
        for j in range(LE):
            weights[w][j].wait()
    for c in sent:
        c.wait_recv()
    for d in range(E):
        rows_all[d * cap : (d + 1) * cap, :] = rows_in[d, 0:cap, :].astype(F32)
    rows = rows_all[...].astype(BF16)

    def product(v, y, c):
        j = lax.div(y, quarters)
        at = c * half + lax.rem(y, quarters) * LANES
        block = v[j, :, pl.ds(pl.multiple_of(at, LANES), LANES)]
        return jnp.dot(rows, block, preferred_element_type=F32)

    to_core = {}
    for o in y_order + [0]:
        for w, v in enumerate((gate_v, up_v)):
            core_out[o, w] = product(v, y_at(o), 1 - core).astype(BF16)
        c = remote(core_out.at[o], core_in.at[o], core_s.at[o], core_r.at[o], me, partner)
        c.start()
        to_core[o] = c
    to_y = {}
    for o in y_order:
        mine = [product(v, y_at(o), core) for v in (gate_v, up_v)]
        to_core[o].wait_recv()
        for w in range(2):
            y_out[o, w] = (mine[w] + core_in[o, w].astype(F32)).astype(BF16)
        c = remote(
            y_out.at[o], y_in.at[o], y_s.at[o], y_r.at[o], me, y_at(o) * CORES + core,
        )
        c.start()
        to_y[o] = c
    mine = [product(v, my, core) for v in (gate_v, up_v)]
    to_core[0].wait_recv()
    gate = mine[0] + core_in[0, 0].astype(F32)
    up = mine[1] + core_in[0, 1].astype(F32)

    for d in range(E):
        block = rows_in[d].astype(F32)
        share_row = block[cap : cap + 1, :] + block[cap + 1 : cap + 2, :]
        info_all[d * cap : (d + 1) * cap, :] = jnp.broadcast_to(share_row, (cap, LANES))
    rlane = iota((R, LANES), 1)
    rslot = lax.rem(iota((R, LANES), 0), cap)
    info_rows = info_all[...]
    share_of = []
    for j in range(LE):
        which = lax.rem(me * LE + j, EPG)
        share_of.append(
            jnp.sum(jnp.where(rlane == which * cap + rslot, info_rows, 0.0), axis=1, keepdims=True)
        )
    finder = jnp.where(key_col == spot_f, 1.0, 0.0)

    for o in reversed(y_order):
        to_y[o].wait_recv()
        gate += y_in[o, 0].astype(F32)
        up += y_in[o, 1].astype(F32)
    hidden = (gate / (1.0 + jnp.exp(-gate)) * up).astype(BF16)
    hid_own[my] = hidden
    to_hid = {}
    for o in y_order:
        c = remote(
            hid_own.at[my], hid_own.at[my], hid_s.at[o], hid_r.at[o], me, y_at(o) * CORES + core,
        )
        c.start()
        to_hid[o] = c
    passed = []

    def forward(o):
        at = lax.rem(my + NY - o, NY)
        c = remote(hid_own.at[at], hid_other.at[at], pass_s.at[o], pass_r.at[o], me, partner)
        c.start()
        passed.append(c)

    forward(0)
    for o in reversed(y_order):
        to_hid[o].wait_recv()
        forward(o)
    for j in range(LE):
        weights[2][j].wait()

    def down(j, held, c):
        joined = jnp.concatenate([held[j * quarters + q] for q in range(quarters)], axis=1)
        part = down_v[j, pl.ds(pl.multiple_of(c * half, half), half), :]
        return jnp.dot(joined, part, preferred_element_type=F32)

    partial = [down(j, hid_own, core) for j in range(LE)]
    for c in passed:
        c.wait_recv()
    total = jnp.zeros((R, width), F32)
    for j in range(LE):
        expert = partial[j] + down(j, hid_other, 1 - core)
        total += share_of[j] * expert.astype(BF16).astype(F32)
    for d in range(E):
        back_out[d] = total[d * cap : (d + 1) * cap, :].astype(BF16)
    back = []
    for d in ep_order:
        c = remote(
            back_out.at[d], back_in.at[me], back_s.at[d], back_r.at[d], source(d), mt,
        )
        c.start()
        back.append(c)
    back_in[me] = back_out[0]
    for c in told + sent + list(to_core.values()) + list(to_y.values()):
        c.wait_send()
    for c in list(to_hid.values()) + passed:
        c.wait_send()
    for c in back:
        c.wait_recv()
    mixed = jnp.zeros((n, width), F32)
    for g in range(G):
        part = back_in[g * group_devices].astype(F32)
        for p in range(1, group_devices):
            part += back_in[g * group_devices + p].astype(F32)
        for s in range(cap):
            at = g * cap + s
            mixed += finder[:, at : at + 1] * part[s : s + 1, :]
    out_ref[...] = mixed
    for c in back:
        c.wait_send()


def per_device(E, T, tokens, norm_gain, norm_bias, group_pick, member_pick, picked_probs,
               gate_weight, up_weight, down_weight):
    n, width = tokens.shape
    LE, _, FF = gate_weight.shape
    NY = T // CORES
    G = LE * E // EPG
    cap = max(n // 4, (n + G - 1) // G)
    R = E * cap
    k = picked_probs.shape[1]
    dma = pltpu.SemaphoreType.DMA
    V = pltpu.VMEM
    scratch = [
        V((n, width), BF16), V((1, width), F32), V((1, width), F32),
        V((1, n), jnp.int32), V((k, n), jnp.int32), V((k, n), F32),
        V((LE, width, FF), BF16), V((LE, width, FF), BF16), V((LE, FF, width), BF16),
        V((1, LANES), F32), V((T, 1, LANES), F32),
        V((G, cap + 2, width), BF16), V((E, cap + 2, width), BF16), V((R, width), F32), V((R, LANES), F32),
        V((NY, 2, R, LANES), BF16), V((NY, 2, R, LANES), BF16),
        V((NY, 2, R, LANES), BF16), V((NY, 2, R, LANES), BF16),
        V((NY, R, LANES), BF16), V((NY, R, LANES), BF16),
        V((E, cap, width), BF16), V((E, cap, width), BF16),
        dma((6,)), dma((3, LE)),
        dma((T,)), dma((T,)), dma((E,)), dma((E,)),
        dma((NY,)), dma((NY,)), dma((NY,)), dma((NY,)), dma((NY,)), dma((NY,)), dma((NY,)), dma((NY,)),
        dma((E,)), dma((E,)),
    ]
    anywhere = pl.BlockSpec(memory_space=pl.ANY)
    combined = pl.pallas_call(
        functools.partial(kernel, E, T, G, cap),
        out_shape=jax.ShapeDtypeStruct((n, width), F32),
        in_specs=[anywhere] * 9,
        out_specs=pl.BlockSpec(memory_space=pltpu.VMEM),
        scratch_shapes=scratch,
        compiler_params=pltpu.CompilerParams(collective_id=0, has_side_effects=True),
        name="moe_step",
    )(tokens, norm_gain.reshape(1, width), norm_bias.reshape(1, width), group_pick.T, member_pick.T,
      picked_probs.T, gate_weight, up_weight, down_weight)
    return combined.astype(BF16)


def solution(mesh):
    placed = (
        P("ep", "tp"), P("tp"), P("tp"), P("ep", None), P("ep", None), P("ep", None),
        P("ep", "tp", None), P("ep", "tp", None), P("ep", None, "tp"),
    )
    body = functools.partial(per_device, mesh.shape["ep"], mesh.shape["tp"])
    return jax.shard_map(body, mesh=mesh, in_specs=placed, out_specs=P("ep", "tp"), check_vma=False)
```

```python
import functools

import jax
import jax.numpy as jnp
from jax import lax
from jax.experimental import pallas as pl
from jax.experimental.pallas import tpu as pltpu
from jax.sharding import PartitionSpec as P

EPG = 8
CORES = 2
LANES = 128
ROW_CHIPS = 4
norm_epsilon = 1e-05
MESH = pl.DeviceIdType.MESH
F32 = jnp.float32
BF16 = jnp.bfloat16


def iota(shape, dim):
    return lax.broadcasted_iota(jnp.int32, shape, dim)


def around(d, size):
    return min(d, size - d)


def kernel(
    E, T, G, cap,
    tokens_h, gain_h, bias_h, group_h, member_h, probs_h, gate_h, up_h, down_h,
    out_ref,
    tokens_v, norm_v, norm_in, group_v, member_v, probs_v, wide_v, down_v,
    stats_out, stats_in, packed_v, rows_v, info_out, info_in, info_all,
    sums_out, sums_in, spread_v, y_out, y_in, hid, expert_v, back_v,
    local_sem, weight_sem, own_sem, swap_s, swap_r,
    stats_s, stats_r, rows_s, rows_r, info_s, info_r, sums_s, sums_r,
    y_s, y_r, hid_s, hid_r, back_s, back_r,
):
    n, width = tokens_h.shape
    NY = T // CORES
    R = E * cap
    group_devices = EPG // CORES
    X = ROW_CHIPS
    Z = E // X
    me = lax.axis_index("ep")
    mt = lax.axis_index("tp")
    core = lax.rem(mt, CORES)
    my = lax.div(mt, CORES)
    mz = lax.div(me, X)
    mx = lax.rem(me, X)
    partner = my * CORES + (1 - core)

    def peer(d):
        dz, dx = divmod(d, X)
        return lax.rem(mz + dz, Z) * X + lax.rem(mx + dx, X)

    def source(d):
        dz, dx = divmod(d, X)
        return lax.rem(mz + Z - dz, Z) * X + lax.rem(mx + X - dx, X)

    def remote(src, dst, ssem, rsem, ep, tp):
        return pltpu.make_async_remote_copy(
            src_ref=src, dst_ref=dst, send_sem=ssem, recv_sem=rsem,
            device_id=(ep, tp), device_id_type=MESH,
        )

    def y_at(o):
        return lax.rem(my + o, NY)

    ep_order = sorted(range(1, E), key=lambda d: -(around(d // X, Z) + around(d % X, X)))
    y_order = sorted(range(1, NY), key=lambda o: -around(o, NY))
    tp_order = sorted(range(1, T), key=lambda t: -around(t // CORES, NY))
    cores = (mt, partner)
    eps = {d: peer(d) for d in ep_order}
    tps = {t: y_at(t // CORES) * CORES + lax.rem(core + t % CORES, CORES) for t in tp_order}

    barrier = pltpu.get_barrier_semaphore()
    for d in ep_order:
        for tp in cores:
            pl.semaphore_signal(barrier, inc=1, device_id=(eps[d], tp), device_id_type=MESH)
    for t in tp_order:
        pl.semaphore_signal(barrier, inc=1, device_id=(me, tps[t]), device_id_type=MESH)

    small = [
        pltpu.make_async_copy(h, v, local_sem.at[i])
        for i, (h, v) in enumerate(
            ((tokens_h, tokens_v), (gain_h, norm_v.at[0]), (bias_h, norm_v.at[1]), (group_h, group_v),
             (member_h, member_v), (probs_h, probs_v))
        )
    ]
    for c in small:
        c.start()
    near = pl.ds(0, width)
    far = pl.ds(width, width)
    weights = [
        pltpu.make_async_copy(gate_h.at[core], wide_v.at[0, near, :], weight_sem.at[0]),
        pltpu.make_async_copy(up_h.at[core], wide_v.at[1, near, :], weight_sem.at[1]),
        pltpu.make_async_copy(down_h.at[core], down_v.at[:, near], weight_sem.at[2]),
    ]
    for c in weights:
        c.start()
    for c in small:
        c.wait()

    lane = iota((n, n), 1)
    sub = iota((n, n), 0)
    spot = iota((n, LANES), 1)

    values = tokens_v[...].astype(F32)
    center_here = jnp.sum(values, axis=1, keepdims=True) / width
    away = values - center_here
    square_here = jnp.sum(away * away, axis=1, keepdims=True)
    stats = jnp.where(spot < LANES // 2, center_here, square_here)
    stats_out[...] = stats
    shifted = (away * norm_v[0]).astype(BF16).astype(F32)

    def column(row):
        wide = jnp.broadcast_to(row, (n, n))
        return jnp.sum(jnp.where(lane == sub, wide, 0.0), axis=1, keepdims=True)

    group_row = group_v[...].astype(F32)
    group_col = column(group_row)
    same = jnp.where(group_col == group_row, 1.0, 0.0)
    slot_row = jnp.sum(jnp.where(sub < lane, same, 0.0), axis=0, keepdims=True)
    slot_col = jnp.sum(jnp.where(lane < sub, same, 0.0), axis=1, keepdims=True)
    place = jnp.where(iota((G * cap, n), 0).astype(F32) == group_row * cap + slot_row, 1.0, 0.0)
    packed = place[:, 0:1] * shifted[0:1, :]
    for t in range(1, n):
        packed += place[:, t : t + 1] * shifted[t : t + 1, :]
    packed_v[...] = packed

    pl.semaphore_wait(barrier, CORES * (E - 1) + T - 1)

    def group_rows(ep):
        return packed_v.at[pl.ds(lax.div(ep, group_devices) * cap, cap), :]

    def slot_rows(d, rel):
        return rows_v.at[pl.ds(d * cap, cap), pl.ds(rel * width, width)]

    sent = []
    for d in ep_order:
        for rel, tp in enumerate(cores):
            c = remote(
                group_rows(eps[d]), slot_rows(d, rel), rows_s.at[rel, d], rows_r.at[rel, d], eps[d], tp,
            )
            c.start()
            sent.append(c)
    c = remote(group_rows(me), slot_rows(0, 1), rows_s.at[1, 0], rows_r.at[1, 0], me, partner)
    c.start()
    sent.append(c)
    own_rows = pltpu.make_async_copy(group_rows(me), slot_rows(0, 0), own_sem.at[0])
    own_rows.start()
    told = []
    for t in tp_order:
        c = remote(stats_out, stats_in.at[t], stats_s.at[t], stats_r.at[t], me, tps[t])
        c.start()
        told.append(c)
    swaps = [
        remote(norm_v, norm_in, swap_s.at[0], swap_r.at[0], me, partner),
        remote(gate_h.at[1 - core], wide_v.at[0, far, :], swap_s.at[1], swap_r.at[1], me, partner),
        remote(up_h.at[1 - core], wide_v.at[1, far, :], swap_s.at[2], swap_r.at[2], me, partner),
        remote(down_h.at[1 - core], down_v.at[:, far], swap_s.at[3], swap_r.at[3], me, partner),
    ]
    for c in swaps:
        c.start()

    probs = probs_v[...]
    member = member_v[...].astype(F32)
    shares = probs / jnp.sum(probs, axis=0, keepdims=True)
    back_lane = iota((n, 2 * R), 1)
    back_slot = lax.rem(back_lane, cap).astype(F32)
    back_ep = lax.div(lax.rem(back_lane, R), cap)
    back_group = lax.div(back_ep, group_devices).astype(F32)
    back_core = jnp.where(back_lane < R, core, 1 - core)
    back_member = (lax.rem(back_ep, group_devices) * CORES + back_core).astype(F32)
    mixing = jnp.zeros((n, 2 * R), F32)
    for k in range(probs.shape[0]):
        mixing += jnp.where(back_member == column(member[k : k + 1, :]), column(shares[k : k + 1, :]), 0.0)
    here = jnp.where(back_group == group_col, 1.0, 0.0) * jnp.where(back_slot == slot_col, 1.0, 0.0)
    mixing = mixing * here
    mixing_high = mixing.astype(BF16).astype(F32)
    mixing = jnp.concatenate([mixing_high, mixing - mixing_high], axis=0).astype(BF16)

    spread_v[...] = jnp.zeros(spread_v.shape, F32)
    for c in weights[:2]:
        c.wait()
    for c in swaps[:3]:
        c.wait_recv()
    gains = (norm_v[0], norm_in[0])
    biases = (norm_v[1], norm_in[1])
    row16 = iota((16, width), 0)

    def factors(w, rel):
        total = jnp.zeros((16, width), F32)
        for at, v in ((2 * rel, gains[rel]), (4, biases[rel])):
            high = v.astype(BF16).astype(F32)
            total += jnp.where(row16 == at + w, high, 0.0) + jnp.where(row16 == at + w + 8, v - high, 0.0)
        return total

    sums = jnp.zeros((16, wide_v.shape[2]), F32)
    for w in range(2):
        both = jnp.concatenate([factors(w, 0), factors(w, 1)], axis=1).astype(BF16)
        sums += jnp.dot(both, wide_v[w], preferred_element_type=F32)
    sums = sums[0:8, :] + sums[8:16, :]
    for y in range(NY):
        sums_out[y] = sums[:, y * LANES : (y + 1) * LANES]
    to_sums = {}
    for o in y_order:
        c = remote(
            sums_out.at[y_at(o)], sums_in.at[o], sums_s.at[o], sums_r.at[o], me, y_at(o) * CORES + core,
        )
        c.start()
        to_sums[o] = c
    sums_in[0] = sums_out[my]

    own_rows.wait()
    for c in sent:
        c.wait_recv()
    rows = rows_v[...].astype(BF16)

    def product(w, y):
        block = wide_v[w, :, pl.ds(pl.multiple_of(y * LANES, LANES), LANES)]
        return jnp.dot(rows, block, preferred_element_type=F32)

    to_y = {}
    for o in y_order:
        for w in range(2):
            y_out[o, w] = product(w, y_at(o)).astype(BF16)
        c = remote(
            y_out.at[o], y_in.at[o], y_s.at[o], y_r.at[o], me, y_at(o) * CORES + core,
        )
        c.start()
        to_y[o] = c

    for c in told:
        c.wait_recv()
    heard = [stats] + [stats_in[t] for t in range(1, T)]
    total = heard[0]
    for h in heard[1:]:
        total += h
    center = total / T
    moved = jnp.zeros((n, LANES), F32)
    for h in heard:
        moved += (h - center) * (h - center)
    inner = jnp.where(spot == 0, width * moved, 0.0) + jnp.where(spot == LANES // 2, total, 0.0)
    spread = jnp.sum(inner, axis=1, keepdims=True) / (width * T)
    factor = lax.rsqrt(spread + norm_epsilon)
    spot_f = spot.astype(F32)
    info = jnp.where(spot_f == slot_col, factor, 0.0)
    for k in range(T):
        info += jnp.where(spot_f == slot_col + (k + 1) * cap, (heard[k] - center) * factor, 0.0)
    for g in range(G):
        info_out[g] = jnp.sum(jnp.where(group_col == g, info, 0.0), axis=0, keepdims=True)
    to_info = {}
    for d in ep_order:
        c = remote(
            info_out.at[lax.div(eps[d], group_devices)], info_in.at[d], info_s.at[d], info_r.at[d], eps[d], mt,
        )
        c.start()
        to_info[d] = c
    info_in[0] = info_out[lax.div(me, group_devices)]

    gate = product(0, my)
    up = product(1, my)

    for o in y_order:
        to_sums[o].wait_recv()
    base_gate = jnp.zeros((1, LANES), F32)
    base_up = jnp.zeros((1, LANES), F32)
    for o in range(NY):
        block = sums_in[o]
        for rel in range(CORES):
            at = (2 * o + rel + 1) * cap
            for w in range(2):
                line = block[2 * rel + w : 2 * rel + w + 1, :]
                spread_v[w, at : at + cap, :] = jnp.broadcast_to(line, (cap, LANES))
        base_gate += block[4:5, :]
        base_up += block[5:6, :]
    for d in ep_order:
        to_info[d].wait_recv()
    for d in range(E):
        info_all[d * cap : (d + 1) * cap, :] = jnp.broadcast_to(info_in[d], (cap, LANES))
    rlane = iota((R, LANES), 1)
    rslot = lax.rem(iota((R, LANES), 0), cap)
    facts = jnp.where(lax.rem(rlane, cap) == rslot, info_all[...], 0.0)
    scale = jnp.sum(jnp.where(rlane < cap, facts, 0.0), axis=1, keepdims=True)

    def extra(w):
        return jnp.dot(facts, spread_v[w], preferred_element_type=F32, precision=lax.Precision.HIGHEST)

    extra_gate = extra(0) + base_gate
    extra_up = extra(1) + base_up

    for o in reversed(y_order):
        to_y[o].wait_recv()
        gate += y_in[o, 0].astype(F32)
        up += y_in[o, 1].astype(F32)
    gate = gate * scale + extra_gate
    up = up * scale + extra_up
    hid[my] = (gate / (1.0 + jnp.exp(-gate)) * up).astype(BF16)
    to_hid = {}
    for o in y_order:
        c = remote(
            hid.at[my], hid.at[my], hid_s.at[o], hid_r.at[o], me, y_at(o) * CORES + core,
        )
        c.start()
        to_hid[o] = c
    weights[2].wait()
    swaps[3].wait_recv()

    def down(o):
        at = lax.rem(my + NY - o, NY)
        block = down_v[pl.ds(pl.multiple_of(at * LANES, LANES), LANES), :]
        return jnp.dot(hid[at], block, preferred_element_type=F32)

    expert = down(0)
    for o in reversed(y_order):
        to_hid[o].wait_recv()
        expert += down(o)
    expert_v[...] = expert.astype(BF16).astype(F32)

    def expert_rows(d, rel):
        return expert_v.at[pl.ds(d * cap, cap), pl.ds(rel * width, width)]

    def back_rows(rel):
        return back_v.at[pl.ds(rel * R + me * cap, cap), :]

    back = []
    for d in ep_order:
        to = source(d)
        for rel, tp in enumerate(cores):
            c = remote(expert_rows(d, rel), back_rows(rel), back_s.at[rel, d], back_r.at[rel, d], to, tp)
            c.start()
            back.append(c)
    c = remote(expert_rows(0, 1), back_rows(1), back_s.at[1, 0], back_r.at[1, 0], me, partner)
    c.start()
    back.append(c)
    own_back = pltpu.make_async_copy(expert_rows(0, 0), back_rows(0), own_sem.at[1])
    own_back.start()
    for c in sent + told + swaps:
        c.wait_send()
    for held in (to_sums, to_y, to_info, to_hid):
        for c in held.values():
            c.wait_send()
    own_back.wait()
    for c in back:
        c.wait_recv()
    mixed = jnp.dot(mixing, back_v[...].astype(BF16), preferred_element_type=F32)
    out_ref[...] = mixed[0:n, :] + mixed[n : 2 * n, :]
    for c in back:
        c.wait_send()


def per_device(E, T, tokens, norm_gain, norm_bias, group_pick, member_pick, picked_probs,
               gate_weight, up_weight, down_weight):
    n, width = tokens.shape
    LE, _, FF = gate_weight.shape
    NY = T // CORES
    G = LE * E // EPG
    cap = max(n // 4, (n + G - 1) // G)
    R = E * cap
    k = picked_probs.shape[1]
    dma = pltpu.SemaphoreType.DMA
    V = pltpu.VMEM
    scratch = [
        V((n, width), BF16), V((2, 1, width), F32), V((2, 1, width), F32),
        V((1, n), jnp.int32), V((k, n), jnp.int32), V((k, n), F32),
        V((2, 2 * width, FF), BF16), V((FF, 2 * width), BF16),
        V((n, LANES), F32), V((T, n, LANES), F32), V((G * cap, width), F32), V((R, 2 * width), F32),
        V((G, 1, LANES), F32), V((E, 1, LANES), F32), V((R, LANES), F32),
        V((NY, 8, LANES), F32), V((NY, 8, LANES), F32), V((2, LANES, LANES), F32),
        V((NY, 2, R, LANES), BF16), V((NY, 2, R, LANES), BF16),
        V((NY, R, LANES), BF16), V((R, 2 * width), F32), V((2 * R, width), F32),
        dma((6,)), dma((3,)), dma((2,)), dma((4,)), dma((4,)),
        dma((T,)), dma((T,)), dma((2, E)), dma((2, E)), dma((E,)), dma((E,)), dma((NY,)), dma((NY,)),
        dma((NY,)), dma((NY,)), dma((NY,)), dma((NY,)), dma((2, E)), dma((2, E)),
    ]
    anywhere = pl.BlockSpec(memory_space=pl.ANY)
    combined = pl.pallas_call(
        functools.partial(kernel, E, T, G, cap),
        out_shape=jax.ShapeDtypeStruct((n, width), F32),
        in_specs=[anywhere] * 9,
        out_specs=pl.BlockSpec(memory_space=pltpu.VMEM),
        scratch_shapes=scratch,
        compiler_params=pltpu.CompilerParams(collective_id=0, has_side_effects=True),
        name="moe_step",
    )(tokens, norm_gain.reshape(1, width), norm_bias.reshape(1, width), group_pick.T, member_pick.T,
      picked_probs.T, gate_weight, up_weight, down_weight)
    return combined.astype(BF16)


def solution(mesh):
    placed = (
        P("ep", "tp"), P("tp"), P("tp"), P("ep", None), P("ep", None), P("ep", None),
        P("ep", "tp", None), P("ep", "tp", None), P("ep", None, "tp"),
    )
    body = functools.partial(per_device, mesh.shape["ep"], mesh.shape["tp"])
    return jax.shard_map(body, mesh=mesh, in_specs=placed, out_specs=P("ep", "tp"), check_vma=False)
```

```python
import functools

import jax
import jax.numpy as jnp
from jax import lax
from jax.experimental import pallas as pl
from jax.experimental.pallas import tpu as pltpu
from jax.sharding import PartitionSpec as P

EPG = 8
CORES = 2
LANES = 128
ROW_CHIPS = 4
norm_epsilon = 1e-05
MESH = pl.DeviceIdType.MESH
F32 = jnp.float32
BF16 = jnp.bfloat16


def iota(shape, dim):
    return lax.broadcasted_iota(jnp.int32, shape, dim)


def around(d, size):
    return min(d, size - d)


def kernel(
    E, T, G, cap,
    tokens_h, gain_h, bias_h, group_h, member_h, probs_h, gate_h, up_h, down_h,
    out_ref,
    tokens_v, norm_v, norm_in, group_v, member_v, probs_v, wide_v, down_v,
    stats_out, stats_in, packed_v, rows_v, info_out, info_in, info_all,
    sums_out, sums_in, spread_v, y_out, y_in, hid, expert_v, back_v,
    local_sem, weight_sem, swap_s, swap_r,
    stats_s, stats_r, rows_s, rows_r, info_s, info_r, sums_s, sums_r,
    y_s, y_r, hid_s, hid_r, back_s, back_r,
):
    n, width = tokens_h.shape
    NY = T // CORES
    R = E * cap
    group_devices = EPG // CORES
    X = ROW_CHIPS
    Z = E // X
    me = lax.axis_index("ep")
    mt = lax.axis_index("tp")
    core = lax.rem(mt, CORES)
    my = lax.div(mt, CORES)
    mz = lax.div(me, X)
    mx = lax.rem(me, X)
    partner = my * CORES + (1 - core)

    def peer(d):
        dz, dx = divmod(d, X)
        return lax.rem(mz + dz, Z) * X + lax.rem(mx + dx, X)

    def source(d):
        dz, dx = divmod(d, X)
        return lax.rem(mz + Z - dz, Z) * X + lax.rem(mx + X - dx, X)

    def remote(src, dst, ssem, rsem, ep, tp):
        return pltpu.make_async_remote_copy(
            src_ref=src, dst_ref=dst, send_sem=ssem, recv_sem=rsem,
            device_id=(ep, tp), device_id_type=MESH,
        )

    def y_at(o):
        return lax.rem(my + o, NY)

    def await_all(ref, sem):
        pltpu.make_async_copy(ref, ref, sem).wait()

    ep_order = sorted(range(1, E), key=lambda d: -(around(d // X, Z) + around(d % X, X)))
    y_order = sorted(range(1, NY), key=lambda o: -around(o, NY))
    tp_order = sorted(range(1, T), key=lambda t: -around(t // CORES, NY))
    cores = (mt, partner)
    eps = {d: peer(d) for d in ep_order}
    tps = {t: y_at(t // CORES) * CORES + lax.rem(core + t % CORES, CORES) for t in tp_order}

    barrier = pltpu.get_barrier_semaphore()
    for d in ep_order:
        for tp in cores:
            pl.semaphore_signal(barrier, inc=1, device_id=(eps[d], tp), device_id_type=MESH)
    for t in tp_order:
        pl.semaphore_signal(barrier, inc=1, device_id=(me, tps[t]), device_id_type=MESH)

    small = [
        pltpu.make_async_copy(h, v, local_sem.at[i])
        for i, (h, v) in enumerate(
            ((tokens_h, tokens_v), (gain_h, norm_v.at[0]), (bias_h, norm_v.at[1]), (group_h, group_v),
             (member_h, member_v), (probs_h, probs_v))
        )
    ]
    for c in small:
        c.start()
    near = pl.ds(0, width)
    far = pl.ds(width, width)
    weights = [
        pltpu.make_async_copy(gate_h.at[core], wide_v.at[0, near, :], weight_sem.at[0]),
        pltpu.make_async_copy(up_h.at[core], wide_v.at[1, near, :], weight_sem.at[1]),
        pltpu.make_async_copy(down_h.at[core], down_v.at[:, near], weight_sem.at[2]),
    ]
    for c in weights:
        c.start()
    for c in small:
        c.wait()

    lane = iota((n, n), 1)
    sub = iota((n, n), 0)
    spot = iota((n, LANES), 1)

    values = tokens_v[...].astype(F32)
    center_here = jnp.sum(values, axis=1, keepdims=True) / width
    away = values - center_here
    square_here = jnp.sum(away * away, axis=1, keepdims=True)
    stats = jnp.where(spot < LANES // 2, center_here, square_here)
    stats_out[...] = stats
    shifted = (away * norm_v[0]).astype(BF16).astype(F32)

    def column(row):
        wide = jnp.broadcast_to(row, (n, n))
        return jnp.sum(jnp.where(lane == sub, wide, 0.0), axis=1, keepdims=True)

    group_row = group_v[...].astype(F32)
    group_col = column(group_row)
    same = jnp.where(group_col == group_row, 1.0, 0.0)
    slot_row = jnp.sum(jnp.where(sub < lane, same, 0.0), axis=0, keepdims=True)
    slot_col = jnp.sum(jnp.where(lane < sub, same, 0.0), axis=1, keepdims=True)
    place = jnp.where(iota((G * cap, n), 0).astype(F32) == group_row * cap + slot_row, 1.0, 0.0)
    packed = place[:, 0:1] * shifted[0:1, :]
    for t in range(1, n):
        packed += place[:, t : t + 1] * shifted[t : t + 1, :]
    packed_v[...] = packed

    pl.semaphore_wait(barrier, CORES * (E - 1) + T - 1)

    def group_rows(ep):
        return packed_v.at[pl.ds(lax.div(ep, group_devices) * cap, cap), :]

    def slot_rows(d, rel):
        return rows_v.at[pl.ds(d * cap, cap), pl.ds(rel * width, width)]

    for d in ep_order:
        for rel, tp in enumerate(cores):
            c = remote(
                group_rows(eps[d]), slot_rows(d, rel), rows_s, rows_r, eps[d], tp,
            )
            c.start()
    c = remote(group_rows(me), slot_rows(0, 1), rows_s, rows_r, me, partner)
    c.start()
    own_rows = pltpu.make_async_copy(group_rows(me), slot_rows(0, 0), rows_r)
    own_rows.start()
    for t in tp_order:
        c = remote(stats_out, stats_in.at[t], stats_s, stats_r, me, tps[t])
        c.start()
    swaps = [
        remote(norm_v, norm_in, swap_s.at[0], swap_r.at[0], me, partner),
        remote(gate_h.at[1 - core], wide_v.at[0, far, :], swap_s.at[1], swap_r.at[1], me, partner),
        remote(up_h.at[1 - core], wide_v.at[1, far, :], swap_s.at[2], swap_r.at[2], me, partner),
        remote(down_h.at[1 - core], down_v.at[:, far], swap_s.at[3], swap_r.at[3], me, partner),
    ]
    for c in swaps:
        c.start()

    probs = probs_v[...]
    member = member_v[...].astype(F32)
    shares = probs / jnp.sum(probs, axis=0, keepdims=True)
    back_lane = iota((n, 2 * R), 1)
    back_slot = lax.rem(back_lane, cap).astype(F32)
    back_ep = lax.div(lax.rem(back_lane, R), cap)
    back_group = lax.div(back_ep, group_devices).astype(F32)
    back_core = jnp.where(back_lane < R, core, 1 - core)
    back_member = (lax.rem(back_ep, group_devices) * CORES + back_core).astype(F32)
    mixing = jnp.zeros((n, 2 * R), F32)
    for k in range(probs.shape[0]):
        mixing += jnp.where(back_member == column(member[k : k + 1, :]), column(shares[k : k + 1, :]), 0.0)
    here = jnp.where(back_group == group_col, 1.0, 0.0) * jnp.where(back_slot == slot_col, 1.0, 0.0)
    mixing = mixing * here
    mixing_high = mixing.astype(BF16).astype(F32)
    mixing = jnp.concatenate([mixing_high, mixing - mixing_high], axis=0).astype(BF16)

    spread_v[...] = jnp.zeros(spread_v.shape, F32)
    for c in weights[:2]:
        c.wait()
    for c in swaps[:3]:
        c.wait_recv()
    gains = (norm_v[0], norm_in[0])
    biases = (norm_v[1], norm_in[1])
    row16 = iota((16, width), 0)

    def factors(w, rel):
        total = jnp.zeros((16, width), F32)
        for at, v in ((2 * rel, gains[rel]), (4, biases[rel])):
            high = v.astype(BF16).astype(F32)
            total += jnp.where(row16 == at + w, high, 0.0) + jnp.where(row16 == at + w + 8, v - high, 0.0)
        return total

    sums = jnp.zeros((16, wide_v.shape[2]), F32)
    for w in range(2):
        both = jnp.concatenate([factors(w, 0), factors(w, 1)], axis=1).astype(BF16)
        sums += jnp.dot(both, wide_v[w], preferred_element_type=F32)
    sums = sums[0:8, :] + sums[8:16, :]
    for y in range(NY):
        sums_out[y] = sums[:, y * LANES : (y + 1) * LANES]
    for o in y_order:
        c = remote(
            sums_out.at[y_at(o)], sums_in.at[o], sums_s, sums_r, me, y_at(o) * CORES + core,
        )
        c.start()
    sums_in[0] = sums_out[my]

    await_all(rows_v, rows_r)
    rows = rows_v[...].astype(BF16)

    def product(w, y):
        block = wide_v[w, :, pl.ds(pl.multiple_of(y * LANES, LANES), LANES)]
        return jnp.dot(rows, block, preferred_element_type=F32)

    for o in y_order:
        for w in range(2):
            y_out[o, w] = product(w, y_at(o)).astype(BF16)
        c = remote(
            y_out.at[o], y_in.at[o], y_s, y_r, me, y_at(o) * CORES + core,
        )
        c.start()

    await_all(stats_in.at[pl.ds(1, T - 1)], stats_r)
    heard = [stats] + [stats_in[t] for t in range(1, T)]
    total = heard[0]
    for h in heard[1:]:
        total += h
    center = total / T
    moved = jnp.zeros((n, LANES), F32)
    for h in heard:
        moved += (h - center) * (h - center)
    inner = jnp.where(spot == 0, width * moved, 0.0) + jnp.where(spot == LANES // 2, total, 0.0)
    spread = jnp.sum(inner, axis=1, keepdims=True) / (width * T)
    factor = lax.rsqrt(spread + norm_epsilon)
    spot_f = spot.astype(F32)
    info = jnp.where(spot_f == slot_col, factor, 0.0)
    for k in range(T):
        info += jnp.where(spot_f == slot_col + (k + 1) * cap, (heard[k] - center) * factor, 0.0)
    for g in range(G):
        info_out[g] = jnp.sum(jnp.where(group_col == g, info, 0.0), axis=0, keepdims=True)
    for d in ep_order:
        c = remote(
            info_out.at[lax.div(eps[d], group_devices)], info_in.at[d], info_s, info_r, eps[d], mt,
        )
        c.start()
    info_in[0] = info_out[lax.div(me, group_devices)]

    gate = product(0, my)
    up = product(1, my)

    await_all(sums_in.at[pl.ds(1, NY - 1)], sums_r)
    base_gate = jnp.zeros((1, LANES), F32)
    base_up = jnp.zeros((1, LANES), F32)
    for o in range(NY):
        block = sums_in[o]
        for rel in range(CORES):
            at = (2 * o + rel + 1) * cap
            for w in range(2):
                line = block[2 * rel + w : 2 * rel + w + 1, :]
                spread_v[w, at : at + cap, :] = jnp.broadcast_to(line, (cap, LANES))
        base_gate += block[4:5, :]
        base_up += block[5:6, :]
    await_all(info_in.at[pl.ds(1, E - 1)], info_r)
    for d in range(E):
        info_all[d * cap : (d + 1) * cap, :] = jnp.broadcast_to(info_in[d], (cap, LANES))
    rlane = iota((R, LANES), 1)
    rslot = lax.rem(iota((R, LANES), 0), cap)
    facts = jnp.where(lax.rem(rlane, cap) == rslot, info_all[...], 0.0)
    scale = jnp.sum(jnp.where(rlane < cap, facts, 0.0), axis=1, keepdims=True)

    def extra(w):
        return jnp.dot(facts, spread_v[w], preferred_element_type=F32, precision=lax.Precision.HIGHEST)

    extra_gate = extra(0) + base_gate
    extra_up = extra(1) + base_up

    await_all(y_in.at[pl.ds(1, NY - 1)], y_r)
    for o in range(1, NY):
        gate += y_in[o, 0].astype(F32)
        up += y_in[o, 1].astype(F32)
    gate = gate * scale + extra_gate
    up = up * scale + extra_up
    hid[my] = (gate / (1.0 + jnp.exp(-gate)) * up).astype(BF16)
    to_hid = {}
    for o in y_order:
        c = remote(
            hid.at[my], hid.at[my], hid_s, hid_r.at[o], me, y_at(o) * CORES + core,
        )
        c.start()
        to_hid[o] = c
    weights[2].wait()
    swaps[3].wait_recv()

    def down(o):
        at = lax.rem(my + NY - o, NY)
        block = down_v[pl.ds(pl.multiple_of(at * LANES, LANES), LANES), :]
        return jnp.dot(hid[at], block, preferred_element_type=F32)

    expert = down(0)
    for o in reversed(y_order):
        to_hid[o].wait_recv()
        expert += down(o)
    expert_v[...] = expert.astype(BF16).astype(F32)

    def expert_rows(d, rel):
        return expert_v.at[pl.ds(d * cap, cap), pl.ds(rel * width, width)]

    def back_rows(rel):
        return back_v.at[pl.ds(rel * R + me * cap, cap), :]

    for d in ep_order:
        to = source(d)
        for rel, tp in enumerate(cores):
            c = remote(expert_rows(d, rel), back_rows(rel), back_s, back_r, to, tp)
            c.start()
    c = remote(expert_rows(0, 1), back_rows(1), back_s, back_r, me, partner)
    c.start()
    own_back = pltpu.make_async_copy(expert_rows(0, 0), back_rows(0), back_r)
    own_back.start()
    for c in swaps:
        c.wait_send()
    await_all(back_v.at[pl.ds(0, 2 * R - cap), :], rows_s)
    await_all(stats_in.at[pl.ds(1, T - 1)], stats_s)
    await_all(sums_in.at[pl.ds(1, NY - 1)], sums_s)
    await_all(info_in.at[pl.ds(1, E - 1)], info_s)
    await_all(y_in.at[pl.ds(1, NY - 1)], y_s)
    await_all(hid.at[pl.ds(1, NY - 1)], hid_s)
    await_all(back_v, back_r)
    mixed = jnp.dot(mixing, back_v[...].astype(BF16), preferred_element_type=F32)
    out_ref[...] = mixed[0:n, :] + mixed[n : 2 * n, :]
    await_all(back_v.at[pl.ds(0, 2 * R - cap), :], back_s)


def per_device(E, T, tokens, norm_gain, norm_bias, group_pick, member_pick, picked_probs,
               gate_weight, up_weight, down_weight):
    n, width = tokens.shape
    LE, _, FF = gate_weight.shape
    NY = T // CORES
    G = LE * E // EPG
    cap = max(n // 4, (n + G - 1) // G)
    R = E * cap
    k = picked_probs.shape[1]
    dma = pltpu.SemaphoreType.DMA
    V = pltpu.VMEM
    scratch = [
        V((n, width), BF16), V((2, 1, width), F32), V((2, 1, width), F32),
        V((1, n), jnp.int32), V((k, n), jnp.int32), V((k, n), F32),
        V((2, 2 * width, FF), BF16), V((FF, 2 * width), BF16),
        V((n, LANES), F32), V((T, n, LANES), F32), V((G * cap, width), F32), V((R, 2 * width), F32),
        V((G, 1, LANES), F32), V((E, 1, LANES), F32), V((R, LANES), F32),
        V((NY, 8, LANES), F32), V((NY, 8, LANES), F32), V((2, LANES, LANES), F32),
        V((NY, 2, R, LANES), BF16), V((NY, 2, R, LANES), BF16),
        V((NY, R, LANES), BF16), V((R, 2 * width), F32), V((2 * R, width), F32),
        dma((6,)), dma((3,)), dma((4,)), dma((4,)),
        dma, dma, dma, dma, dma, dma, dma, dma,
        dma, dma, dma, dma((NY,)), dma, dma,
    ]
    anywhere = pl.BlockSpec(memory_space=pl.ANY)
    combined = pl.pallas_call(
        functools.partial(kernel, E, T, G, cap),
        out_shape=jax.ShapeDtypeStruct((n, width), F32),
        in_specs=[anywhere] * 9,
        out_specs=pl.BlockSpec(memory_space=pltpu.VMEM),
        scratch_shapes=scratch,
        compiler_params=pltpu.CompilerParams(collective_id=0, has_side_effects=True),
        name="moe_step",
    )(tokens, norm_gain.reshape(1, width), norm_bias.reshape(1, width), group_pick.T, member_pick.T,
      picked_probs.T, gate_weight, up_weight, down_weight)
    return combined.astype(BF16)


def solution(mesh):
    placed = (
        P("ep", "tp"), P("tp"), P("tp"), P("ep", None), P("ep", None), P("ep", None),
        P("ep", "tp", None), P("ep", "tp", None), P("ep", None, "tp"),
    )
    body = functools.partial(per_device, mesh.shape["ep"], mesh.shape["tp"])
    return jax.shard_map(body, mesh=mesh, in_specs=placed, out_specs=P("ep", "tp"), check_vma=False)
```
